128 devices in a mesh: sp: 32 (over y, x, core), tp: 4 (over z).
Axes of the slice: x: 4, y: 4, z: 4, core: 2. Of those that a mesh axis runs over, the one named last changes fastest.
Arguments:
- sequence: bfloat16 [4, 1024, 1024], P(None, 'sp', 'tp'), may hold values from -6 to 6
- norm_gain: float32 [3, 1024], replicated, may hold values from 0.1 to 1.9
- weight_value: bfloat16 [3, 1024, 512], P(None, 'sp', 'tp'), may hold values from -0.1875 to 0.1875
- weight_outer: bfloat16 [3, 1024, 512], P(None, 'sp', 'tp'), may hold values from -0.1875 to 0.1875
- weight_inner: bfloat16 [3, 1024, 512], P(None, 'sp', 'tp'), may hold values from -0.1875 to 0.1875
- conv_taps: float32 [3, 3, 512], P(None, None, 'tp'), may hold values from -3 to 3
- weight_out: bfloat16 [3, 512, 1024], P(None, 'tp', 'sp'), may hold values from -0.25 to 0.25
Outputs:
- mixed: bfloat16 [4, 1024, 1024], P(None, 'sp', 'tp')
The draws below stay inside these ranges and needn't reach their ends.
All inputs are finite; a program needn't handle non-finite values.
Results may differ from the reference program's by a relative error of at most 0.03.
Values may be sent and summed in bfloat16 or wider, within the bound.
A program may use at most 64 MiB of HBM per device.

```python
import jax
import jax.numpy as jnp
from jax import lax

D = 1024
CW = 512
KTAPS = 3
LAYERS = 3
SEQS = 4
TOKENS = 1024


def level_of(stream_key, extent, shards, smallest, largest):
    def one(position, parts):
        heights = jax.random.uniform(jax.random.fold_in(jax.random.fold_in(stream_key, 6), position), (parts,), jnp.float32, smallest / len(shards), largest / len(shards))
        return jnp.repeat(jnp.exp(heights), extent[position] // parts).reshape((-1,) + (1,) * (len(extent) - position - 1))

    gain = one(*shards[0])
    for cut in shards[1:]:
        gain = gain * one(*cut)
    return gain


def noise(rng, shape, deviation, bound, cuts=(), dtype=jnp.bfloat16):
    level = level_of(rng, shape, cuts, -0.22, 0.18) if cuts else 1.0
    entries = jax.random.normal(rng, shape, jnp.float32) * deviation * level
    return jnp.minimum(jnp.maximum(entries, -bound), bound).astype(dtype)


def setup_inputs(seed: int = 0) -> dict:
    seeds = jax.random.split(jax.random.key(seed), 8)
    sequence = noise(seeds[0], (SEQS, TOKENS, D), 1.0, 6.0, ((1, 32), (2, 4)))
    norm_gain = jnp.clip(1.0 + 0.18 * jax.random.normal(seeds[1], (LAYERS, D), jnp.float32), 0.1, 1.9)
    weight_value = noise(seeds[2], (LAYERS, D, CW), D ** -0.5, 0.1875, ((1, 32), (2, 4)))
    weight_outer = noise(seeds[3], (LAYERS, D, CW), D ** -0.5, 0.1875, ((1, 32), (2, 4)))
    weight_inner = noise(seeds[4], (LAYERS, D, CW), D ** -0.5, 0.1875, ((1, 32), (2, 4)))
    conv_taps = noise(seeds[5], (LAYERS, KTAPS, CW), 0.6, 3.0, ((2, 4),), jnp.float32)
    weight_out = noise(seeds[6], (LAYERS, CW, D), CW ** -0.5, 0.25, ((1, 4), (2, 32)))
    return {"sequence": sequence, "norm_gain": norm_gain, "weight_value": weight_value, "weight_outer": weight_outer, "weight_inner": weight_inner, "conv_taps": conv_taps, "weight_out": weight_out}


def rms_rows(values, gain_row):
    wide = values.astype(jnp.float32)
    scaled = wide * lax.rsqrt(lax.optimization_barrier(jnp.mean(wide * wide, axis=-1, keepdims=True)) + 1e-06)
    return (scaled * gain_row).astype(jnp.bfloat16)

def reference(sequence, norm_gain, weight_value, weight_outer, weight_inner, conv_taps, weight_out):
    current = sequence
    for layer_index in range(LAYERS):
        normed = rms_rows(current, norm_gain[layer_index]).reshape(SEQS * TOKENS, D)
        proj_value = jnp.dot(normed, weight_value[layer_index], preferred_element_type=jnp.float32).astype(jnp.bfloat16)
        proj_outer = jnp.dot(normed, weight_outer[layer_index], preferred_element_type=jnp.float32).astype(jnp.bfloat16)
        proj_inner = jnp.dot(normed, weight_inner[layer_index], preferred_element_type=jnp.float32).astype(jnp.bfloat16)
        product = (proj_inner.astype(jnp.float32) * proj_value.astype(jnp.float32)).reshape(SEQS, TOKENS, CW)
        padded = jnp.pad(product, ((0, 0), (KTAPS - 1, 0), (0, 0)))
        filtered = conv_taps[layer_index, 0] * padded[:, 0:TOKENS]
        for offset in range(1, KTAPS):
            filtered = filtered + conv_taps[layer_index, offset] * padded[:, offset:offset + TOKENS]
        gated = (proj_outer.astype(jnp.float32).reshape(SEQS, TOKENS, CW) * filtered).astype(jnp.bfloat16)
        projected = jnp.dot(gated.reshape(SEQS * TOKENS, CW), weight_out[layer_index], preferred_element_type=jnp.float32)
        current = (current.astype(jnp.float32) + projected.reshape(SEQS, TOKENS, D)).astype(jnp.bfloat16)
    return current
```

```python
import functools

import jax
import jax.numpy as jnp
from jax import lax
from jax.experimental import pallas as pl
from jax.experimental.pallas import tpu as pltpu
from jax.sharding import PartitionSpec as P

MESH = pl.DeviceIdType.MESH
LAYERS = 3
HALO = 8
SEQS = 4
LOCAL = 32
SPAN = LOCAL + HALO
ROWS = SEQS * SPAN
D = 1024
BF = jnp.bfloat16
F32 = jnp.float32
SEMS = 192


def kernel(seq, gain, wv, wo, wi, taps, wout, out, IN, OUT, XG, HG, GX, CUR, NORM, lsem, ssem, rsem):
    sp = lax.axis_index("sp")
    z = lax.axis_index("tp")
    c = lax.rem(sp, 2)
    x = lax.rem(sp // 2, 4)
    y = sp // 8

    def dev(dx=0, dy=0, dz=0, dc=0):
        xx = lax.rem(x + dx + 4, 4)
        yy = lax.rem(y + dy + 4, 4)
        cc = lax.rem(c + dc, 2)
        return ((yy * 4 + xx) * 2 + cc, lax.rem(z + dz + 4, 4))

    succ = (lax.rem(sp + 1, 32), z)
    pred = (lax.rem(sp + 31, 32), z)
    partner = dev(dc=1)

    def at(i, step):
        return lax.rem(i + step + 4, 4)

    place = ((y, x), (x, y))
    local = []
    for col in range(2):
        i, j = place[col]
        for m, w in enumerate((wv, wo, wi)):
            local.append(
                pltpu.make_async_copy(
                    w.at[:, pl.ds(16 * col, 16), :], IN.at[:, c, col, i, j, m], lsem.at[len(local)]
                )
            )
            local[-1].start()
    xcopy = pltpu.make_async_copy(seq, XG.at[z], lsem.at[len(local)])
    xcopy.start()

    for layer in range(LAYERS):
        turned = jnp.transpose(wout[layer].astype(F32)).astype(BF)
        for col in range(2):
            i, j = place[col]
            OUT[layer, c, col, i, j, z] = turned[16 * col : 16 * col + 16]

    barrier = pltpu.get_barrier_semaphore()
    friends = [dev(dx=1), dev(dx=-1), dev(dx=2), dev(dy=1), dev(dy=-1), dev(dy=2)]
    friends += [dev(dz=1), dev(dz=-1), dev(dz=2), partner, succ, pred]
    for friend in friends:
        pl.semaphore_signal(barrier, inc=1, device_id=friend, device_id_type=MESH)
    pl.semaphore_wait(barrier, len(friends))

    sent = {}

    def send(key, src, dst, target):
        k = len(sent)
        copy = pltpu.make_async_remote_copy(
            src_ref=src,
            dst_ref=dst,
            send_sem=ssem.at[k],
            recv_sem=rsem.at[k],
            device_id=target,
            device_id_type=MESH,
        )
        copy.start()
        sent[key] = copy

    def share(key, ref, target):
        send(key, ref, ref, target)

    def arrived(key):
        sent[key].wait_recv()

    def peer(col, di, dj):
        return dev(dx=dj, dy=di) if col == 0 else dev(dx=di, dy=dj)

    BUF = {"i": IN, "o": OUT}

    def unit_first(unit):
        buf, layer = BUF[unit[0]], unit[1]
        for col in range(2):
            i, j = place[col]
            for step in (1, -1, 2):
                share((unit, col, "p1", step), buf.at[layer, c, col, i, j], peer(col, 0, step))

    def unit_a(unit):
        buf, layer = BUF[unit[0]], unit[1]
        for col in range(2):
            i, j = place[col]
            for step in (1, -1, 2):
                arrived((unit, col, "p1", step))
            row = buf.at[layer, c, col, i]
            for step in (1, -1):
                share((unit, col, "p2", step), row, peer(col, step, 0))
            share((unit, col, "d", 0), row, partner)

    def unit_b(unit):
        buf, layer = BUF[unit[0]], unit[1]
        for col in range(2):
            i, j = place[col]
            for step in (1, -1):
                arrived((unit, col, "p2", step))
                row = at(i, -step)
                half = pl.ds(0 if step == 1 else 2, 2)
                share((unit, col, "p3", step), buf.at[layer, c, col, row, half], peer(col, step, 0))
                share((unit, col, "d", step), buf.at[layer, c, col, row], partner)

    def unit_c(unit):
        buf, layer = BUF[unit[0]], unit[1]
        for col in range(2):
            i, j = place[col]
            row = at(i, 2)
            for step in (1, -1):
                arrived((unit, col, "p3", step))
            share((unit, col, "d", 2), buf.at[layer, c, col, row], partner)

    def unit_d(unit):
        for col in range(2):
            for step in (0, 1, -1, 2):
                arrived((unit, col, "d", step))

    for copy in local:
        copy.wait()
    unit_first(("i", 0))
    xcopy.wait()
    for step in (1, -1, 2):
        share(("x", step), XG.at[z], dev(dz=step))
    send("halo", XG.at[z, :, pl.ds(16, 16), :], HG.at[z], succ)
    for col in range(2):
        i, j = place[col]
        for step in (1, -1, 2):
            share(("wo", col, step), OUT.at[:, c, col, i, j, z], dev(dz=step))
    unit_first(("i", 1))
    unit_first(("i", 2))

    unit_a(("i", 0))
    arrived("halo")
    for step in (1, -1, 2):
        share(("h", step), HG.at[z], dev(dz=step))
    for col in range(2):
        for step in (1, -1, 2):
            arrived(("wo", col, step))
    unit_first(("o", 0))
    unit_a(("i", 1))
    unit_b(("i", 0))
    unit_first(("o", 1))
    unit_first(("o", 2))
    unit_a(("o", 0))
    unit_c(("i", 0))

    for step in (1, -1, 2):
        arrived(("x", step))
        arrived(("h", step))
    first = jnp.where(sp == 0, 0.0, 1.0).astype(F32)
    for s in range(SEQS):
        for zz in range(4):
            columns = pl.ds(256 * zz, 256)
            before = HG[zz, s].astype(F32)[16 - HALO :]
            CUR[pl.ds(SPAN * s, HALO), columns] = before * first
            CUR[pl.ds(SPAN * s + HALO, LOCAL), columns] = XG[zz, s].astype(F32)

    def normalise(layer):
        for r in range(0, ROWS, 32):
            wide = CUR[pl.ds(r, 32), :]
            scaled = wide * lax.rsqrt(jnp.mean(wide * wide, axis=-1, keepdims=True) + 1e-06)
            NORM[pl.ds(r, 32), :] = (scaled * gain[pl.ds(layer, 1), :]).astype(BF)

    def gate(layer):
        total = jnp.zeros((ROWS, 384), F32)
        for yy in range(4):
            tiles = []
            for xx in range(4):
                for cc in range(2):
                    for col in range(2):
                        i, j = (yy, xx) if col == 0 else (xx, yy)
                        tiles.append(
                            jnp.concatenate([IN[layer, cc, col, i, j, m] for m in range(3)], axis=1)
                        )
            weights = jnp.concatenate(tiles, axis=0)
            total = total + jnp.dot(
                NORM[:, pl.ds(256 * yy, 256)], weights, preferred_element_type=F32
            )
        total = total.astype(BF).astype(F32)
        value, outer, inner = total[:, :128], total[:, 128:256], total[:, 256:]
        product = inner * value
        filtered = taps[layer, pl.ds(0, 1), :] * pltpu.roll(product, 2, 0)
        filtered = filtered + taps[layer, pl.ds(1, 1), :] * pltpu.roll(product, 1, 0)
        filtered = filtered + taps[layer, pl.ds(2, 1), :] * product
        GX[layer, z] = (outer * filtered).astype(BF)
        for step in (1, -1, 2):
            share(("g", layer, step), GX.at[layer, z], dev(dz=step))

    def project(layer):
        for step in (1, -1, 2):
            arrived(("g", layer, step))
        gated = jnp.concatenate([GX[layer, zz] for zz in range(4)], axis=1)
        last = layer == LAYERS - 1

        def columns_of(yy):
            tiles = []
            for xx in range(4):
                for cc in range(2):
                    for col in range(2):
                        i, j = (yy, xx) if col == 0 else (xx, yy)
                        tiles.append(
                            jnp.concatenate([OUT[layer, cc, col, i, j, zz] for zz in range(4)], axis=1)
                        )
            weights = jnp.concatenate(tiles, axis=0)
            return lax.dot_general(
                gated, weights, (((1,), (1,)), ((), ())), preferred_element_type=F32
            )

        if last:
            total = columns_of(z)
            mine = pl.ds(pl.multiple_of(256 * z, 256), 256)
            total = CUR[:, mine] + total
            for s in range(SEQS):
                out[s] = total[SPAN * s + HALO : SPAN * (s + 1)].astype(BF)
        else:
            for yy in range(4):
                columns = pl.ds(256 * yy, 256)
                CUR[:, columns] = (CUR[:, columns] + columns_of(yy)).astype(BF).astype(F32)

    normalise(0)
    unit_d(("i", 0))
    gate(0)

    unit_b(("i", 1))
    unit_a(("i", 2))
    unit_b(("o", 0))
    unit_a(("o", 1))
    unit_c(("i", 1))
    unit_c(("o", 0))
    unit_d(("o", 0))
    project(0)
    normalise(1)
    unit_d(("i", 1))
    gate(1)

    unit_b(("o", 1))
    unit_a(("o", 2))
    unit_b(("i", 2))
    unit_c(("o", 1))
    unit_c(("i", 2))
    unit_d(("o", 1))
    project(1)
    normalise(2)
    unit_d(("i", 2))
    gate(2)

    unit_b(("o", 2))
    unit_c(("o", 2))
    unit_d(("o", 2))
    project(2)

    for copy in sent.values():
        copy.wait_send()


def body(sequence, norm_gain, weight_value, weight_outer, weight_inner, conv_taps, weight_out):
    anywhere = pl.BlockSpec(memory_space=pl.ANY)
    vmem = pl.BlockSpec(memory_space=pltpu.VMEM)
    return pl.pallas_call(
        kernel,
        out_shape=jax.ShapeDtypeStruct(sequence.shape, BF),
        in_specs=[anywhere, vmem, anywhere, anywhere, anywhere, vmem, vmem],
        out_specs=vmem,
        scratch_shapes=[
            pltpu.VMEM((LAYERS, 2, 2, 4, 4, 3, 16, 128), BF),
            pltpu.VMEM((LAYERS, 2, 2, 4, 4, 4, 16, 128), BF),
            pltpu.VMEM((4, SEQS, LOCAL, 256), BF),
            pltpu.VMEM((4, SEQS, 16, 256), BF),
            pltpu.VMEM((LAYERS, 4, ROWS, 128), BF),
            pltpu.VMEM((ROWS, D), F32),
            pltpu.VMEM((ROWS, D), BF),
            pltpu.SemaphoreType.DMA((8,)),
            pltpu.SemaphoreType.DMA((SEMS,)),
            pltpu.SemaphoreType.DMA((SEMS,)),
        ],
        compiler_params=pltpu.CompilerParams(collective_id=0, has_side_effects=True),
    )(sequence, norm_gain, weight_value, weight_outer, weight_inner, conv_taps, weight_out)


def solution(mesh):
    return jax.shard_map(
        body,
        mesh=mesh,
        in_specs=(
            P(None, "sp", "tp"),
            P(),
            P(None, "sp", "tp"),
            P(None, "sp", "tp"),
            P(None, "sp", "tp"),
            P(None, None, "tp"),
            P(None, "tp", "sp"),
        ),
        out_specs=P(None, "sp", "tp"),
        check_vma=False,
    )
```

```python
import functools

import jax
import jax.numpy as jnp
from jax import lax
from jax.experimental import pallas as pl
from jax.experimental.pallas import tpu as pltpu
from jax.sharding import PartitionSpec as P

MESH = pl.DeviceIdType.MESH
LAYERS = 3
HALO = 8
SEQS = 4
LOCAL = 32
SPAN = LOCAL + HALO
ROWS = SEQS * SPAN
D = 1024
BF = jnp.bfloat16
F32 = jnp.float32
SEMS = 192


def kernel(seq, gain, wv, wo, wi, taps, wout, out, IN, OUT, XG, HG, GX, CUR, NORM, lsem, ssem, rsem):
    sp = lax.axis_index("sp")
    z = lax.axis_index("tp")
    c = lax.rem(sp, 2)
    x = lax.rem(sp // 2, 4)
    y = sp // 8

    def dev(dx=0, dy=0, dz=0, dc=0):
        xx = lax.rem(x + dx + 4, 4)
        yy = lax.rem(y + dy + 4, 4)
        cc = lax.rem(c + dc, 2)
        return ((yy * 4 + xx) * 2 + cc, lax.rem(z + dz + 4, 4))

    succ = (lax.rem(sp + 1, 32), z)
    pred = (lax.rem(sp + 31, 32), z)
    partner = dev(dc=1)

    def at(i, step):
        return lax.rem(i + step + 4, 4)

    place = ((y, x), (x, y))
    local = []
    for col in range(2):
        i, j = place[col]
        for m, w in enumerate((wv, wo, wi)):
            local.append(
                pltpu.make_async_copy(
                    w.at[:, pl.ds(16 * col, 16), :], IN.at[:, c, col, i, j, m], lsem.at[len(local)]
                )
            )
            local[-1].start()
    weigh = []
    for col in range(2):
        i, j = place[col]
        weigh.append(
            pltpu.make_async_copy(
                wout.at[:, pl.ds(16 * col, 16), :], OUT.at[:, c, col, i, j, z], lsem.at[len(local) + col]
            )
        )
        weigh[-1].start()
    xcopy = pltpu.make_async_copy(seq, XG.at[z], lsem.at[8])
    xcopy.start()

    barrier = pltpu.get_barrier_semaphore()
    friends = [dev(dx=1), dev(dx=-1), dev(dx=2), dev(dy=1), dev(dy=-1), dev(dy=2)]
    friends += [dev(dz=1), dev(dz=-1), dev(dz=2), partner, succ, pred]
    for friend in friends:
        pl.semaphore_signal(barrier, inc=1, device_id=friend, device_id_type=MESH)
    pl.semaphore_wait(barrier, len(friends))

    sent = {}

    def send(key, src, dst, target):
        k = len(sent)
        copy = pltpu.make_async_remote_copy(
            src_ref=src,
            dst_ref=dst,
            send_sem=ssem.at[k],
            recv_sem=rsem.at[k],
            device_id=target,
            device_id_type=MESH,
        )
        copy.start()
        sent[key] = copy

    def share(key, ref, target):
        send(key, ref, ref, target)

    def arrived(key):
        sent[key].wait_recv()

    def peer(col, di, dj):
        return dev(dx=dj, dy=di) if col == 0 else dev(dx=di, dy=dj)

    BUF = {"i": IN, "o": OUT}

    def unit_first(unit):
        buf, layer = BUF[unit[0]], unit[1]
        for col in range(2):
            i, j = place[col]
            for step in (1, -1, 2):
                share((unit, col, "p1", step), buf.at[layer, c, col, i, j], peer(col, 0, step))

    def unit_a(unit):
        buf, layer = BUF[unit[0]], unit[1]
        for col in range(2):
            i, j = place[col]
            for step in (1, -1, 2):
                arrived((unit, col, "p1", step))
            row = buf.at[layer, c, col, i]
            for step in (1, -1):
                share((unit, col, "p2", step), row, peer(col, step, 0))
            share((unit, col, "d", 0), row, partner)

    def unit_b(unit):
        buf, layer = BUF[unit[0]], unit[1]
        for col in range(2):
            i, j = place[col]
            for step in (1, -1):
                arrived((unit, col, "p2", step))
                row = at(i, -step)
                half = pl.ds(0 if step == 1 else 2, 2)
                share((unit, col, "p3", step), buf.at[layer, c, col, row, half], peer(col, step, 0))
                share((unit, col, "d", step), buf.at[layer, c, col, row], partner)

    def unit_c(unit):
        buf, layer = BUF[unit[0]], unit[1]
        for col in range(2):
            i, j = place[col]
            row = at(i, 2)
            for step in (1, -1):
                arrived((unit, col, "p3", step))
            share((unit, col, "d", 2), buf.at[layer, c, col, row], partner)

    def unit_d(unit):
        for col in range(2):
            for step in (0, 1, -1, 2):
                arrived((unit, col, "d", step))

    for copy in local:
        copy.wait()
    unit_first(("i", 0))
    xcopy.wait()
    for step in (1, -1, 2):
        share(("x", step), XG.at[z], dev(dz=step))
    send("halo", XG.at[z, :, pl.ds(16, 16), :], HG.at[z], succ)
    for col in range(2):
        weigh[col].wait()
        i, j = place[col]
        for step in (1, -1, 2):
            share(("wo", col, step), OUT.at[:, c, col, i, j, z], dev(dz=step))
    unit_first(("i", 1))
    unit_first(("i", 2))

    unit_a(("i", 0))
    arrived("halo")
    for step in (1, -1, 2):
        share(("h", step), HG.at[z], dev(dz=step))
    for col in range(2):
        for step in (1, -1, 2):
            arrived(("wo", col, step))
    unit_first(("o", 0))
    unit_a(("i", 1))
    unit_b(("i", 0))
    unit_first(("o", 1))
    unit_first(("o", 2))
    unit_a(("o", 0))
    unit_c(("i", 0))

    for step in (1, -1, 2):
        arrived(("x", step))
        arrived(("h", step))
    first = jnp.where(sp == 0, 0.0, 1.0).astype(F32)
    for s in range(SEQS):
        for zz in range(4):
            columns = pl.ds(256 * zz, 256)
            before = HG[zz, s].astype(F32)[16 - HALO :]
            CUR[pl.ds(SPAN * s, HALO), columns] = before * first
            CUR[pl.ds(SPAN * s + HALO, LOCAL), columns] = XG[zz, s].astype(F32)

    def normalise(layer):
        for r in range(0, ROWS, 32):
            wide = CUR[pl.ds(r, 32), :]
            scaled = wide * lax.rsqrt(jnp.mean(wide * wide, axis=-1, keepdims=True) + 1e-06)
            NORM[pl.ds(r, 32), :] = (scaled * gain[pl.ds(layer, 1), :]).astype(BF)

    def gate(layer):
        total = jnp.zeros((ROWS, 384), F32)
        for yy in range(4):
            tiles = []
            for xx in range(4):
                for cc in range(2):
                    for col in range(2):
                        i, j = (yy, xx) if col == 0 else (xx, yy)
                        tiles.append(
                            jnp.concatenate([IN[layer, cc, col, i, j, m] for m in range(3)], axis=1)
                        )
            weights = jnp.concatenate(tiles, axis=0)
            total = total + jnp.dot(
                NORM[:, pl.ds(256 * yy, 256)], weights, preferred_element_type=F32
            )
        total = total.astype(BF).astype(F32)
        value, outer, inner = total[:, :128], total[:, 128:256], total[:, 256:]
        product = inner * value
        filtered = taps[layer, pl.ds(0, 1), :] * pltpu.roll(product, 2, 0)
        filtered = filtered + taps[layer, pl.ds(1, 1), :] * pltpu.roll(product, 1, 0)
        filtered = filtered + taps[layer, pl.ds(2, 1), :] * product
        GX[layer, z] = (outer * filtered).astype(BF)
        for step in (1, -1, 2):
            share(("g", layer, step), GX.at[layer, z], dev(dz=step))

    def project(layer):
        for step in (1, -1, 2):
            arrived(("g", layer, step))
        gated = jnp.concatenate([GX[layer, zz] for zz in range(4)], axis=1)
        last = layer == LAYERS - 1

        def columns_of(yy):
            tiles = []
            for xx in range(4):
                for cc in range(2):
                    for col in range(2):
                        i, j = (yy, xx) if col == 0 else (xx, yy)
                        tiles.append(
                            jnp.concatenate([OUT[layer, cc, col, i, j, zz] for zz in range(4)], axis=1)
                        )
            weights = jnp.concatenate(tiles, axis=0)
            return lax.dot_general(
                gated, weights, (((1,), (1,)), ((), ())), preferred_element_type=F32
            )

        if last:
            total = columns_of(z)
            mine = pl.ds(pl.multiple_of(256 * z, 256), 256)
            total = CUR[:, mine] + total
            for s in range(SEQS):
                out[s] = total[SPAN * s + HALO : SPAN * (s + 1)].astype(BF)
        else:
            for yy in range(4):
                columns = pl.ds(256 * yy, 256)
                CUR[:, columns] = (CUR[:, columns] + columns_of(yy)).astype(BF).astype(F32)

    normalise(0)
    unit_d(("i", 0))
    gate(0)

    unit_b(("i", 1))
    unit_a(("i", 2))
    unit_b(("o", 0))
    unit_a(("o", 1))
    unit_c(("i", 1))
    unit_c(("o", 0))
    unit_d(("o", 0))
    project(0)
    normalise(1)
    unit_d(("i", 1))
    gate(1)

    unit_b(("o", 1))
    unit_a(("o", 2))
    unit_b(("i", 2))
    unit_c(("o", 1))
    unit_c(("i", 2))
    unit_d(("o", 1))
    project(1)
    normalise(2)
    unit_d(("i", 2))
    gate(2)

    unit_b(("o", 2))
    unit_c(("o", 2))
    unit_d(("o", 2))
    project(2)

    for copy in sent.values():
        copy.wait_send()


def body(sequence, norm_gain, weight_value, weight_outer, weight_inner, conv_taps, weight_out):
    anywhere = pl.BlockSpec(memory_space=pl.ANY)
    vmem = pl.BlockSpec(memory_space=pltpu.VMEM)
    return pl.pallas_call(
        kernel,
        out_shape=jax.ShapeDtypeStruct(sequence.shape, BF),
        in_specs=[anywhere, vmem, anywhere, anywhere, anywhere, vmem, anywhere],
        out_specs=vmem,
        scratch_shapes=[
            pltpu.VMEM((LAYERS, 2, 2, 4, 4, 3, 16, 128), BF),
            pltpu.VMEM((LAYERS, 2, 2, 4, 4, 4, 16, 128), BF),
            pltpu.VMEM((4, SEQS, LOCAL, 256), BF),
            pltpu.VMEM((4, SEQS, 16, 256), BF),
            pltpu.VMEM((LAYERS, 4, ROWS, 128), BF),
            pltpu.VMEM((ROWS, D), F32),
            pltpu.VMEM((ROWS, D), BF),
            pltpu.SemaphoreType.DMA((9,)),
            pltpu.SemaphoreType.DMA((SEMS,)),
            pltpu.SemaphoreType.DMA((SEMS,)),
        ],
        compiler_params=pltpu.CompilerParams(collective_id=0, has_side_effects=True),
    )(sequence, norm_gain, weight_value, weight_outer, weight_inner, conv_taps, jnp.swapaxes(weight_out, 1, 2))


def solution(mesh):
    return jax.shard_map(
        body,
        mesh=mesh,
        in_specs=(
            P(None, "sp", "tp"),
            P(),
            P(None, "sp", "tp"),
            P(None, "sp", "tp"),
            P(None, "sp", "tp"),
            P(None, None, "tp"),
            P(None, "tp", "sp"),
        ),
        out_specs=P(None, "sp", "tp"),
        check_vma=False,
    )
```

```python
import functools

import jax
import jax.numpy as jnp
from jax import lax
from jax.experimental import pallas as pl
from jax.experimental.pallas import tpu as pltpu
from jax.sharding import PartitionSpec as P

MESH = pl.DeviceIdType.MESH
LAYERS = 3
HALO = 8
SEQS = 4
LOCAL = 32
SPAN = LOCAL + HALO
ROWS = SEQS * SPAN
D = 1024
BF = jnp.bfloat16
F32 = jnp.float32
SEMS = 48


def kernel(seq, gain, wv, wo, wi, taps, wout, out, IN, OUT, XG, HG, GX, CUR, NORM, GAIN, TAPS, sems):
    sp = lax.axis_index("sp")
    z = lax.axis_index("tp")
    c = lax.rem(sp, 2)
    x = lax.rem(sp // 2, 4)
    y = sp // 8

    def dev(dx=0, dy=0, dz=0, dc=0):
        xx = lax.rem(x + dx + 4, 4)
        yy = lax.rem(y + dy + 4, 4)
        cc = lax.rem(c + dc, 2)
        return ((yy * 4 + xx) * 2 + cc, lax.rem(z + dz + 4, 4))

    succ = (lax.rem(sp + 1, 32), z)
    pred = (lax.rem(sp + 31, 32), z)
    partner = dev(dc=1)
    place = ((y, x), (x, y))
    steps = (1, -1, 2)
    BUF = {"i": IN, "o": OUT}

    def at(i, step):
        return lax.rem(i + step + 4, 4)

    names = {}

    def sem(key):
        return sems.at[names.setdefault(key, len(names))]

    def fetch(key, src, dst):
        pltpu.make_async_copy(src, dst, sem(key)).start()

    def fetched(key, like):
        pltpu.make_async_copy(like, like, sem(key)).wait()

    def send(key, group, src, dst, target):
        pltpu.make_async_remote_copy(
            src_ref=src,
            dst_ref=dst,
            send_sem=sem(("sent", group)),
            recv_sem=sem(key),
            device_id=target,
            device_id_type=MESH,
        ).start()

    def share(key, group, ref, target):
        send(key, group, ref, ref, target)

    def waiter(key, group, like):
        return pltpu.make_async_remote_copy(
            src_ref=like,
            dst_ref=like,
            send_sem=sem(("sent", group)),
            recv_sem=sem(key),
            device_id=partner,
            device_id_type=MESH,
        )

    def arrived(key, group, like):
        waiter(key, group, like).wait_recv()

    def left(key, group, like):
        waiter(key, group, like).wait_send()

    def peer(col, di, dj):
        return dev(dx=dj, dy=di) if col == 0 else dev(dx=di, dy=dj)

    for col in range(2):
        i, j = place[col]
        for m, w in enumerate((wv, wo, wi)):
            fetch("li", w.at[:, pl.ds(16 * col, 16), :], IN.at[:, c, col, i, j, m])
    for col in range(2):
        i, j = place[col]
        fetch("lo", wout.at[:, pl.ds(16 * col, 16), :], OUT.at[:, c, col, i, j, z])
    fetch("lx", seq, XG.at[z])
    fetch("lg", gain, GAIN)
    fetch("lt", taps, TAPS)

    def barrier_step():
        barrier = pltpu.get_barrier_semaphore()
        friends = [dev(dx=1), dev(dx=-1), dev(dx=2), dev(dy=1), dev(dy=-1), dev(dy=2)]
        friends += [dev(dz=1), dev(dz=-1), dev(dz=2), partner, succ, pred]
        for friend in friends:
            pl.semaphore_signal(barrier, inc=1, device_id=friend, device_id_type=MESH)
        pl.semaphore_wait(barrier, len(friends))

    def head_first():
        fetched("li", IN.at[0, 0, 0, pl.ds(0, 2), pl.ds(0, 3)])
        for col in range(2):
            i, j = place[col]
            own = IN.at[0, c, col, i, j]
            for step in steps:
                share("head far" if step == 2 else "head near", "i1", own, peer(col, 0, step))
        for col in range(2):
            i, j = place[col]
            for step in steps:
                share("head early", "i2", IN.at[0, c, col, i, j], peer(col, step, 0))

    def head_near():
        arrived("head near", "i1", IN.at[0, 0, 0, 0])
        for col in range(2):
            i, j = place[col]
            for back in (1, -1):
                for step in steps:
                    share("head early", "i2", IN.at[0, c, col, i, at(j, back)], peer(col, step, 0))

    def head_far():
        arrived("head far", "i1", IN.at[0, 0, 0, 0, pl.ds(0, 2)])
        for col in range(2):
            i, j = place[col]
            for step in steps:
                share("head late", "i2", IN.at[0, c, col, i, at(j, 2)], peer(col, step, 0))
        for col in range(2):
            i, j = place[col]
            share("head twin", "id", IN.at[0, c, col, i], partner)

    def head_rest():
        arrived("head early", "i2", IN.at[0, :, 0, pl.ds(0, 3), pl.ds(0, 3)])
        arrived("head late", "i2", IN.at[0, :, 0, 0, pl.ds(0, 3)])
        for col in range(2):
            i, j = place[col]
            for step in steps:
                share("head twin", "id", IN.at[0, c, col, at(i, step)], partner)

    def head_done():
        arrived("head twin", "id", IN.at[0, 0])

    def first(kind, layer):
        buf = BUF[kind]
        for col in range(2):
            i, j = place[col]
            for step in steps:
                share((kind, layer, 1), kind + "1", buf.at[layer, c, col, i, j], peer(col, 0, step))

    def second(kind, layer):
        buf = BUF[kind]
        arrived((kind, layer, 1), kind + "1", buf.at[layer, :, 0, 0, pl.ds(0, 3)])
        for col in range(2):
            i, j = place[col]
            for step in steps:
                share((kind, layer, 2), kind + "2", buf.at[layer, c, col, i], peer(col, step, 0))

    def third(kind, layer):
        buf = BUF[kind]
        arrived((kind, layer, 2), kind + "2", buf.at[layer, :, 0, pl.ds(0, 3)])
        share((kind, layer, 3), kind + "d", buf.at[layer, c], partner)

    def done(kind, layer):
        arrived((kind, layer, 3), kind + "d", BUF[kind].at[layer, 0])

    def stage_w(layer):
        if layer == 0:
            fetched("lo", OUT.at[0, 0, 0, 0, pl.ds(0, 2), pl.ds(0, 3)])
        for col in range(2):
            i, j = place[col]
            for step in steps:
                share(("w", layer), "w", OUT.at[layer, c, col, i, j, z], dev(dz=step))

    def wait_w(layer):
        arrived(("w", layer), "w", OUT.at[0, 0, 0, 0, pl.ds(0, 2), pl.ds(0, 3)])

    def stage_x():
        fetched("lx", XG.at[0])
        send("halo", "halo", XG.at[z, :, pl.ds(16, 16), :], HG.at[z], succ)
        for step in steps:
            share("x", "x", XG.at[z], dev(dz=step))

    def stage_h():
        arrived("halo", "halo", HG.at[0])
        for step in steps:
            share("h", "h", HG.at[z], dev(dz=step))

    def wait_x():
        arrived("x", "x", XG.at[pl.ds(0, 3)])
        arrived("h", "h", HG.at[pl.ds(0, 3)])
        fetched("lg", GAIN)
        fetched("lt", TAPS)

    def gwait(layer):
        arrived(("g", layer), "g", GX.at[0, pl.ds(0, 3)])

    def finish():
        left("x", "x", XG.at[pl.ds(0, 3)])
        left("h", "h", HG.at[pl.ds(0, 3)])
        left("halo", "halo", HG.at[0])
        left(("g", 0), "g", GX.at[:, pl.ds(0, 3)])
        left(("w", 0), "w", OUT.at[:, 0, 0, 0, pl.ds(0, 2), pl.ds(0, 3)])
        for kind in "io":
            buf = BUF[kind]
            left((kind, 1, 1), kind + "1", buf.at[:, :, 0, 0, pl.ds(0, 3)])
            left((kind, 1, 2), kind + "2", buf.at[:, :, 0, pl.ds(0, 3)])
            left((kind, 1, 3), kind + "d", buf.at[:, 0])

    def assemble():
        begun = jnp.where(sp == 0, 0.0, 1.0).astype(F32)
        for s in range(SEQS):
            for zz in range(4):
                columns = pl.ds(256 * zz, 256)
                before = HG[zz, s].astype(F32)[16 - HALO :]
                CUR[pl.ds(SPAN * s, HALO), columns] = before * begun
                CUR[pl.ds(SPAN * s + HALO, LOCAL), columns] = XG[zz, s].astype(F32)

    def normalise(layer):
        for r in range(0, ROWS, 32):
            wide = CUR[pl.ds(r, 32), :]
            scaled = wide * lax.rsqrt(jnp.mean(wide * wide, axis=-1, keepdims=True) + 1e-06)
            NORM[pl.ds(r, 32), :] = (scaled * GAIN[pl.ds(layer, 1), :]).astype(BF)

    def gate(layer):
        total = jnp.zeros((ROWS, 384), F32)
        for yy in range(4):
            tiles = []
            for xx in range(4):
                for cc in range(2):
                    for col in range(2):
                        i, j = (yy, xx) if col == 0 else (xx, yy)
                        tiles.append(
                            jnp.concatenate([IN[layer, cc, col, i, j, m] for m in range(3)], axis=1)
                        )
            weights = jnp.concatenate(tiles, axis=0)
            total = total + jnp.dot(
                NORM[:, pl.ds(256 * yy, 256)], weights, preferred_element_type=F32
            )
        total = total.astype(BF).astype(F32)
        value, outer, inner = total[:, :128], total[:, 128:256], total[:, 256:]
        product = inner * value
        filtered = TAPS[layer, pl.ds(0, 1), :] * pltpu.roll(product, 2, 0)
        filtered = filtered + TAPS[layer, pl.ds(1, 1), :] * pltpu.roll(product, 1, 0)
        filtered = filtered + TAPS[layer, pl.ds(2, 1), :] * product
        GX[layer, z] = (outer * filtered).astype(BF)
        for step in (1, -1, 2):
            share(("g", layer), "g", GX.at[layer, z], dev(dz=step))

    def project(layer):
        gated = jnp.concatenate([GX[layer, zz] for zz in range(4)], axis=1)
        last = layer == LAYERS - 1

        def columns_of(yy):
            tiles = []
            for xx in range(4):
                for cc in range(2):
                    for col in range(2):
                        i, j = (yy, xx) if col == 0 else (xx, yy)
                        tiles.append(
                            jnp.concatenate([OUT[layer, cc, col, i, j, zz] for zz in range(4)], axis=1)
                        )
            weights = jnp.concatenate(tiles, axis=0)
            return lax.dot_general(
                gated, weights, (((1,), (1,)), ((), ())), preferred_element_type=F32
            )

        if last:
            total = columns_of(z)
            mine = pl.ds(pl.multiple_of(256 * z, 256), 256)
            total = CUR[:, mine] + total
            for s in range(SEQS):
                out[s] = total[SPAN * s + HALO : SPAN * (s + 1)].astype(BF)
        else:
            for yy in range(4):
                columns = pl.ds(256 * yy, 256)
                CUR[:, columns] = (CUR[:, columns] + columns_of(yy)).astype(BF).astype(F32)

    barrier_step()
    head_first()
    stage_w(0)
    stage_x()
    stage_w(1)
    stage_w(2)
    first("i", 1)
    first("i", 2)
    head_near()
    stage_h()
    head_far()
    wait_w(0)
    first("o", 0)
    second("i", 1)
    wait_w(1)
    first("o", 1)
    wait_w(2)
    first("o", 2)
    wait_x()
    assemble()
    normalise(0)
    head_rest()
    head_done()
    gate(0)
    second("o", 0)
    second("i", 2)
    third("i", 1)
    second("o", 1)
    third("o", 0)
    done("o", 0)
    gwait(0)
    project(0)
    normalise(1)
    done("i", 1)
    gate(1)
    second("o", 2)
    third("i", 2)
    third("o", 1)
    done("o", 1)
    gwait(1)
    project(1)
    normalise(2)
    done("i", 2)
    gate(2)
    third("o", 2)
    done("o", 2)
    gwait(2)
    project(2)
    finish()
    assert len(names) <= SEMS, len(names)


def body(sequence, norm_gain, weight_value, weight_outer, weight_inner, conv_taps, weight_out):
    anywhere = pl.BlockSpec(memory_space=pl.ANY)
    vmem = pl.BlockSpec(memory_space=pltpu.VMEM)
    return pl.pallas_call(
        kernel,
        out_shape=jax.ShapeDtypeStruct(sequence.shape, BF),
        in_specs=[anywhere] * 7,
        out_specs=vmem,
        scratch_shapes=[
            pltpu.VMEM((LAYERS, 2, 2, 4, 4, 3, 16, 128), BF),
            pltpu.VMEM((LAYERS, 2, 2, 4, 4, 4, 16, 128), BF),
            pltpu.VMEM((4, SEQS, LOCAL, 256), BF),
            pltpu.VMEM((4, SEQS, 16, 256), BF),
            pltpu.VMEM((LAYERS, 4, ROWS, 128), BF),
            pltpu.VMEM((ROWS, D), F32),
            pltpu.VMEM((ROWS, D), BF),
            pltpu.VMEM((LAYERS, D), F32),
            pltpu.VMEM((LAYERS, 3, 128), F32),
            pltpu.SemaphoreType.DMA((SEMS,)),
        ],
        compiler_params=pltpu.CompilerParams(collective_id=0, has_side_effects=True),
    )(sequence, norm_gain, weight_value, weight_outer, weight_inner, conv_taps, jnp.swapaxes(weight_out, 1, 2))


def solution(mesh):
    return jax.shard_map(
        body,
        mesh=mesh,
        in_specs=(
            P(None, "sp", "tp"),
            P(),
            P(None, "sp", "tp"),
            P(None, "sp", "tp"),
            P(None, "sp", "tp"),
            P(None, None, "tp"),
            P(None, "tp", "sp"),
        ),
        out_specs=P(None, "sp", "tp"),
        check_vma=False,
    )
```
